128 devices in a mesh: sp: 32 (over z, y, core), tp: 4 (over x).
Axes of the slice: x: 4, y: 4, z: 4, core: 2. Of those that a mesh axis runs over, the one named last changes fastest.
Arguments:
- tokens: bfloat16 [6, 8192, 2048], P(None, 'sp', 'tp'), may hold values from -6 to 6
- norm_gains: float32 [3, 2048], replicated, may hold values from 0.5 to 1.5
- weight_outer: bfloat16 [3, 2048, 1024], P(None, 'sp', 'tp'), may hold values from -0.125 to 0.125
- weight_inner: bfloat16 [3, 2048, 1024], P(None, 'sp', 'tp'), may hold values from -0.125 to 0.125
- weight_value: bfloat16 [3, 2048, 1024], P(None, 'sp', 'tp'), may hold values from -0.125 to 0.125
- conv_taps: bfloat16 [3, 3, 1024], P(None, None, 'tp'), may hold values from -3.5 to 3.5
- weight_output: bfloat16 [3, 1024, 2048], P(None, 'sp', 'tp'), may hold values from -0.1875 to 0.1875
Outputs:
- mixed_out: float32 [6, 8192, 2048], P(None, 'sp', 'tp')
The draws below stay inside these ranges and needn't reach their ends.
All inputs are finite; a program needn't handle non-finite values.
Results may differ from the reference program's by a relative error of at most 0.03.
Values may be sent and summed in bfloat16 or wider, within the bound.
A program may use at most 128 MiB of HBM per device.

```python
import jax
import jax.numpy as jnp
from jax import lax

D = 2048
SC = 1024
KERNEL = 3
LAYERS = 3
SEQS = 6
SEQ = 8192


def shard_levels(key, dims, cuts, smallest, top_value):
    factor_of, own = 1.0, jax.random.fold_in(key, 6)
    for position, shards_of in cuts:
        draws = jnp.exp(jax.random.uniform(jax.random.fold_in(own, position), (shards_of,), jnp.float32, smallest / len(cuts), top_value / len(cuts)))
        factor_of = factor_of * jnp.repeat(draws, dims[position] // shards_of).reshape([-1 if axis == position else 1 for axis in range(len(dims))])
    return factor_of


def centred(stream_key, shape, scale, bound, pieces=(), held_as=jnp.bfloat16):
    values = scale * jax.random.normal(stream_key, shape, jnp.float32)
    if pieces:
        values = values * shard_levels(stream_key, shape, pieces, -0.22, 0.18)
    return jnp.clip(values, -bound, bound).astype(held_as)


def setup_inputs(seed: int = 0) -> dict:
    arg_keys = jax.random.split(jax.random.key(seed), 8)
    return {
        "tokens": centred(arg_keys[0], (SEQS, SEQ, D), 1.0, 6.0, ((1, 32), (2, 4))),
        "norm_gains": jnp.clip(1.0 + 0.1 * jax.random.normal(arg_keys[1], (LAYERS, D), jnp.float32), 0.5, 1.5),
        "weight_outer": centred(arg_keys[2], (LAYERS, D, SC), D ** -0.5, 0.125, ((1, 32), (2, 4))),
        "weight_inner": centred(arg_keys[3], (LAYERS, D, SC), D ** -0.5, 0.125, ((1, 32), (2, 4))),
        "weight_value": centred(arg_keys[4], (LAYERS, D, SC), D ** -0.5, 0.125, ((1, 32), (2, 4))),
        "conv_taps": centred(arg_keys[5], (LAYERS, KERNEL, SC), KERNEL ** -0.5, 3.5, ((2, 4),)),
        "weight_output": centred(arg_keys[6], (LAYERS, SC, D), SC ** -0.5, 0.1875, ((1, 32), (2, 4))),
    }


epsilon = 1e-06

def normalize(values_in, gain_row):
    values = values_in.astype(jnp.float32)
    scale = lax.rsqrt(lax.optimization_barrier(jnp.mean(values * values, axis=-1, keepdims=True)) + epsilon)
    return (values * scale * gain_row.astype(jnp.float32)).astype(jnp.bfloat16)

def reference(tokens, norm_gains, weight_outer, weight_inner, weight_value, conv_taps, weight_output):
    current = tokens
    projected = None
    for layer in range(LAYERS):
        normed = normalize(current, norm_gains[layer]).reshape(SEQS * SEQ, D)
        outer = jnp.dot(normed, weight_outer[layer], preferred_element_type=jnp.float32).astype(jnp.bfloat16)
        inner = jnp.dot(normed, weight_inner[layer], preferred_element_type=jnp.float32).astype(jnp.bfloat16)
        value = jnp.dot(normed, weight_value[layer], preferred_element_type=jnp.float32).astype(jnp.bfloat16)
        outer, inner, value = lax.optimization_barrier((outer, inner, value))
        gated = (inner.astype(jnp.float32) * value.astype(jnp.float32)).reshape(SEQS, SEQ, SC)
        padded = jnp.pad(gated, ((0, 0), (KERNEL - 1, 0), (0, 0)))
        conved = jnp.zeros((SEQS, SEQ, SC), jnp.float32)
        for offset in range(KERNEL):
            conved = conved + conv_taps[layer, offset].astype(jnp.float32) * padded[:, offset:offset + SEQ]
        mixer = (outer.astype(jnp.float32).reshape(SEQS, SEQ, SC) * conved).astype(jnp.bfloat16)
        projected = jnp.dot(mixer.reshape(SEQS * SEQ, SC), weight_output[layer], preferred_element_type=jnp.float32)
        current = projected.astype(jnp.bfloat16).reshape(SEQS, SEQ, D)
    return projected.reshape(SEQS, SEQ, D)
```

```python
import functools

import jax
import jax.numpy as jnp
from jax import lax
from jax.experimental import pallas as pl
from jax.experimental.pallas import tpu as pltpu
from jax.sharding import PartitionSpec as P

MESH = pl.DeviceIdType.MESH
EPS = 1e-06
L = 3
HALO = 16
ROWS_A, ROWS_B = 256, 128
A0 = HALO
B0 = HALO + ROWS_A + HALO
ROWS = B0 + ROWS_B
BF, F32 = jnp.bfloat16, jnp.float32

ORDERS = (
    ("xyz", "xyz", "xzy"),
    ("yzx", "yzx", "yzx"),
    ("zxy", "zxy", "zxy"),
    ("xzy", "xyz", "xyz"),
)
NMAT = 4


class Sems:
    def __init__(self):
        self.at = {}

    def __getitem__(self, key):
        return self.at.setdefault(key, len(self.at))


N_SEMS = 256


def kernel(
    tokens, gains, w_o, w_i, w_v, taps, w_u, out, wx, wu, x_buf, n_buf, m_buf, g_buf, t_buf, send, recv, local
):
    sp, x = lax.axis_index("sp"), lax.axis_index("tp")
    c, y, z = lax.rem(sp, 2), lax.rem(sp // 2, 4), sp // 8
    sems = Sems()
    pending = []
    args = (w_o, w_i, w_v, w_u)

    def device(dx=0, dy=0, dz=0, dc=0):
        sp_of = lax.rem(z + dz + 4, 4) * 8 + lax.rem(y + dy + 4, 4) * 2 + lax.rem(c + dc, 2)
        return (sp_of, lax.rem(x + dx + 4, 4))

    def neighbour(dim, sign):
        return device(**{"d" + dim: sign})

    def remote(src, dst, key, dev):
        k = sems[key]
        return pltpu.make_async_remote_copy(
            src_ref=src, dst_ref=dst, send_sem=send.at[k], recv_sem=recv.at[k], device_id=dev, device_id_type=MESH
        )

    def start(src, dst, key, dev):
        copy = remote(src, dst, key, dev)
        copy.start()
        pending.append(copy)

    def arrived(dst, key):
        remote(dst, dst, key, device(dc=1)).wait_recv()

    def region(m, layer, full, moved=None, by=0, half=None):
        place = {"x": x, "y": y, "z": z}
        if moved is not None:
            place[moved] = lax.rem(place[moved] + by + 4, 4)
        pick = [slice(None) if d in full else place[d] for d in "xzy"]
        rows = 64 if m < 3 else 32
        tail = slice(None) if half is None else pl.ds(half * (rows // 2), rows // 2)
        if m < 3:
            return wx.at[(layer, m, *pick, c, tail)]
        return wu.at[(layer, *pick, c, tail)]

    ALL = slice(None)

    barrier = pltpu.get_barrier_semaphore()
    left_sp, right_sp = lax.rem(sp + 31, 32), lax.rem(sp + 1, 32)
    peers = [device(dx=d) for d in (1, 2, 3)]
    peers += [neighbour(d, s) for d in "yz" for s in (1, -1)]
    peers.append(device(dc=1))
    for d in range(4):
        peers += [(right_sp, lax.rem(x + d, 4)), (left_sp, lax.rem(x + d, 4))]
    for peer in peers:
        pl.semaphore_signal(barrier, inc=1, device_id=peer, device_id_type=MESH)
    g_buf[pl.ds(0, 8), :] = jnp.zeros((8, 256), F32)
    own = []
    for m in range(NMAT):
        own.append(pltpu.make_async_copy(args[m], region(m, ALL, ""), local.at[m]))
        own[-1].start()
    pl.semaphore_wait(barrier, len(peers))

    for m in range(NMAT):
        d = ORDERS[m][0][0]
        for s in (1, -1):
            start(args[m], region(m, ALL, ""), (m, 1, s), neighbour(d, s))

    def rows_of(xd):
        return 3 * (xd // 2) + 2 * lax.rem(xd, 2), 3 * (xd // 2) + 1, lax.rem(xd, 2)

    def token_copies():
        found = []
        for d in range(4):
            xd = lax.rem(x + d, 4)
            seq_a, seq_b, odd = rows_of(xd)
            row_b = pl.multiple_of(128 * odd, 128)
            here = (sp, xd)
            there = (right_sp, xd)
            pieces = [
                (None, tokens.at[seq_a], x_buf.at[x, pl.ds(A0, ROWS_A)], "a", here),
                (None, tokens.at[seq_b, pl.ds(row_b, ROWS_B)], x_buf.at[x, pl.ds(B0, ROWS_B)], "b", here),
                (sp < 31, tokens.at[seq_a, pl.ds(240, 16)], x_buf.at[x, pl.ds(0, 16)], "ha", there),
                ((odd == 0) & (sp < 31), tokens.at[seq_b, pl.ds(240, 16)], x_buf.at[x, pl.ds(B0 - 16, 16)], "he", there),
                (odd == 1, tokens.at[seq_b, pl.ds(112, 16)], x_buf.at[x, pl.ds(B0 - 16, 16)], "ho", here),
            ]
            for when, src, dst, name, dev in pieces:
                key = ("tok", name, d)
                if d == 0 and name in ("a", "b", "ho"):
                    copy = pltpu.make_async_copy(src, dst, local.at[{"a": 4, "b": 5, "ho": 6}[name]])
                    found.append((when, copy, True))
                else:
                    found.append((when, remote(src, dst, key, dev), False))
        return found

    def guarded(when, action):
        if when is None:
            action()
        else:
            pl.when(when)(action)

    pltpu.make_async_copy(taps, t_buf.at[x], local.at[7]).start()
    for d in (1, 2, 3):
        start(taps, t_buf.at[x], ("taps", d), device(dx=d))
    token_list = token_copies()

    def start_tokens():
        for when, copy, _ in token_list:
            guarded(when, copy.start)

    def wait_tokens():
        for when, copy, is_local in token_list:
            if is_local:
                guarded(when, copy.wait)
        odd = lax.rem(x, 2)
        for d in range(4):
            xs = lax.rem(x - d + 4, 4)
            arriving = [
                (None, x_buf.at[xs, pl.ds(A0, ROWS_A)], "a"),
                (None, x_buf.at[xs, pl.ds(B0, ROWS_B)], "b"),
                (sp > 0, x_buf.at[xs, pl.ds(0, 16)], "ha"),
                ((odd == 0) & (sp > 0), x_buf.at[xs, pl.ds(B0 - 16, 16)], "he"),
                (odd == 1, x_buf.at[xs, pl.ds(B0 - 16, 16)], "ho"),
            ]
            for when, dst, name in arriving:
                if d == 0 and name in ("a", "b", "ho"):
                    continue
                guarded(when, functools.partial(arrived, dst, ("tok", name, d)))

        @pl.when(sp == 0)
        def _():
            x_buf[:, pl.ds(0, 16), :] = jnp.zeros((4, 16, 512), BF)

        @pl.when((sp == 0) & (odd == 0))
        def _():
            x_buf[:, pl.ds(B0 - 16, 16), :] = jnp.zeros((4, 16, 512), BF)

        pltpu.make_async_copy(taps, t_buf.at[x], local.at[7]).wait()
        for d in (1, 2, 3):
            arrived(t_buf.at[lax.rem(x - d + 4, 4)], ("taps", d))

    for m in range(NMAT):
        d = ORDERS[m][0][0]
        for s in (1, -1):
            arrived(region(m, ALL, "", d, -s), (m, 1, s))
            part = region(m, ALL, "", d, -s, half=0 if s == 1 else 1)
            start(part, part, (m, 2, s), neighbour(d, s))
    for m in range(NMAT):
        own[m].wait()

    for layer in range(L):
        for m in range(NMAT):
            first, d, _ = ORDERS[m][layer]
            if layer == 0:
                for s in (1, -1):
                    arrived(region(m, ALL, "", first, -2 * s, half=0 if s == 1 else 1), (m, 2, s))
            for s in (1, -1):
                block = region(m, layer, first)
                start(block, block, (m, layer, 3, s), neighbour(d, s))
        if layer == 0:
            start_tokens()
    for layer in range(L):
        for m in range(NMAT):
            first, d, _ = ORDERS[m][layer]
            for s in (1, -1):
                arrived(region(m, layer, first, d, -s), (m, layer, 3, s))
                part = region(m, layer, first, d, -s, half=0 if s == 1 else 1)
                start(part, part, (m, layer, 4, s), neighbour(d, s))

    partner = device(dc=1)

    def second_done(layer):
        for m in range(NMAT):
            first, d, _ = ORDERS[m][layer]
            for s in (1, -1):
                arrived(region(m, layer, first, d, -2 * s, half=0 if s == 1 else 1), (m, layer, 4, s))

    def third(layer, part):
        for m in range(NMAT):
            first, second, d = ORDERS[m][layer]
            for s in (1, -1):
                half = part if s == 1 else 1 - part
                block = region(m, layer, first + second, half=half)
                start(block, block, (m, layer, 5 + part, s), neighbour(d, s))

    def across(layer, which):
        for m in range(NMAT):
            first, second, d = ORDERS[m][layer]
            block = region(m, layer, first + second, d, which)
            start(block, block, (m, layer, "core", which), partner)

    def pass_on(layer):
        for m in range(NMAT):
            first, second, d = ORDERS[m][layer]
            for s in (1, -1):
                part = region(m, layer, first + second, d, -s, half=0 if s == 1 else 1)
                arrived(part, (m, layer, 5, s))
                start(part, part, (m, layer, 7, s), neighbour(d, s))

    def near_done(layer):
        for m in range(NMAT):
            first, second, d = ORDERS[m][layer]
            for s in (1, -1):
                arrived(region(m, layer, first + second, d, -s, half=1 if s == 1 else 0), (m, layer, 6, s))
        across(layer, 1)
        across(layer, -1)

    def far_done(layer):
        for m in range(NMAT):
            first, second, d = ORDERS[m][layer]
            for s in (1, -1):
                arrived(region(m, layer, first + second, d, 2, half=0 if s == 1 else 1), (m, layer, 7, s))
        across(layer, 2)

    def other_core(m, layer, which):
        first, second, d = ORDERS[m][layer]
        place = {"x": x, "y": y, "z": z}
        place[d] = lax.rem(place[d] + which + 4, 4)
        pick = [slice(None) if k != d else place[k] for k in "xzy"]
        return wx.at[(layer, m, *pick, 1 - c)] if m < 3 else wu.at[(layer, *pick, 1 - c)]

    def from_partner(layer):
        for which in (0, 1, -1, 2):
            for m in range(NMAT):
                arrived(other_core(m, layer, which), (m, layer, "core", which))

    def normalize(layer):
        def step(r, _):
            rows = pl.ds(pl.multiple_of(r * 32, 32), 32)
            total = jnp.zeros((32, 1), F32)
            for k in range(4):
                v = x_buf[k, rows, :].astype(F32)
                total += jnp.sum(v * v, axis=-1, keepdims=True)
            scale = lax.rsqrt(total * (1.0 / 2048) + EPS)
            for k in range(4):
                v = x_buf[k, rows, :].astype(F32)
                gain = gains[pl.ds(layer, 1), pl.ds(k * 512, 512)]
                n_buf[rows, pl.ds(k * 512, 512)] = (v * scale * gain).astype(BF)
            return 0

        lax.fori_loop(0, ROWS // 32, step, 0)

    def mix(layer):
        def step(b, _):
            def project(m):
                weight = wx[layer, m, b].reshape(2048, 256)
                return jnp.dot(n_buf[...], weight, preferred_element_type=F32).astype(BF).astype(F32)

            g_buf[pl.ds(8, ROWS), :] = project(1) * project(2)
            outer = project(0)
            conved = jnp.zeros((ROWS, 256), F32)
            for k in range(3):
                conved += t_buf[b, layer, pl.ds(k, 1), :] * g_buf[pl.ds(6 + k, ROWS), :]
            m_buf[:, pl.ds(pl.multiple_of(b * 256, 256), 256)] = (outer * conved).astype(BF)
            return 0

        lax.fori_loop(0, 4, step, 0)

    def project_out(layer, b):
        weight = wu[layer, b].reshape(1024, 512)
        x_buf[b] = jnp.dot(m_buf[...], weight, preferred_element_type=F32).astype(BF)

    def project_all(layer):
        def step(b, _):
            project_out(layer, b)
            return 0

        lax.fori_loop(0, 4, step, 0)

    second_done(0)
    third(0, 0)
    third(0, 1)
    across(0, 0)
    second_done(1)
    third(1, 0)
    across(1, 0)
    second_done(2)
    across(2, 0)
    wait_tokens()
    normalize(0)
    pass_on(0)
    third(1, 1)
    third(2, 0)
    near_done(0)
    far_done(0)
    from_partner(0)
    mix(0)
    project_all(0)
    pass_on(1)
    third(2, 1)
    normalize(1)
    near_done(1)
    far_done(1)
    from_partner(1)
    mix(1)
    project_all(1)
    pass_on(2)
    normalize(2)
    near_done(2)
    far_done(2)
    from_partner(2)
    mix(2)

    seq_a, seq_b, odd = rows_of(x)
    row_b = pl.multiple_of(128 * odd, 128)
    dst_a = out.at[seq_a]
    dst_b = out.at[seq_b, pl.ds(row_b, ROWS_B)]
    for d in (2, 1, 3, 0):
        xd = lax.rem(x + d, 4)
        project_out(L - 1, xd)
        src_a, src_b = x_buf.at[xd, pl.ds(A0, ROWS_A)], x_buf.at[xd, pl.ds(B0, ROWS_B)]
        if d == 0:
            last = [pltpu.make_async_copy(src_a, dst_a, local.at[4]), pltpu.make_async_copy(src_b, dst_b, local.at[5])]
            for copy in last:
                copy.start()
        else:
            start(src_a, dst_a, ("out", "a", d), (sp, xd))
            start(src_b, dst_b, ("out", "b", d), (sp, xd))
    for when, copy, is_local in token_list:
        if not is_local:
            guarded(when, copy.wait_send)
    for copy in pending:
        copy.wait_send()
    for d in (2, 1, 3):
        from_a, from_b, from_odd = rows_of(lax.rem(x - d + 4, 4))
        arrived(out.at[from_a], ("out", "a", d))
        arrived(out.at[from_b, pl.ds(pl.multiple_of(128 * from_odd, 128), ROWS_B)], ("out", "b", d))
    for copy in last:
        copy.wait()
    assert len(sems.at) <= N_SEMS


def body(tokens, norm_gains, weight_outer, weight_inner, weight_value, conv_taps, weight_output):
    taps = jnp.pad(conv_taps.astype(F32), ((0, 0), (0, 5), (0, 0)))
    hbm = pl.BlockSpec(memory_space=pl.ANY)
    vmem = pl.BlockSpec(memory_space=pltpu.VMEM)
    result = pl.pallas_call(
        kernel,
        out_shape=jax.ShapeDtypeStruct((6, 256, 512), BF),
        in_specs=[hbm, vmem, hbm, hbm, hbm, hbm, hbm],
        out_specs=hbm,
        scratch_shapes=[
            pltpu.VMEM((L, 3, 4, 4, 4, 2, 64, 256), BF),
            pltpu.VMEM((L, 4, 4, 4, 2, 32, 512), BF),
            pltpu.VMEM((4, ROWS, 512), BF),
            pltpu.VMEM((ROWS, 2048), BF),
            pltpu.VMEM((ROWS, 1024), BF),
            pltpu.VMEM((ROWS + 8, 256), F32),
            pltpu.VMEM((4, 3, 8, 256), F32),
            pltpu.SemaphoreType.DMA((N_SEMS,)),
            pltpu.SemaphoreType.DMA((N_SEMS,)),
            pltpu.SemaphoreType.DMA((8,)),
        ],
        compiler_params=pltpu.CompilerParams(
            collective_id=0, has_side_effects=True, vmem_limit_bytes=67_000_000
        ),
        name="mixers",
    )(tokens, norm_gains, weight_outer, weight_inner, weight_value, taps, weight_output)
    return result.astype(F32)


def solution(mesh):
    in_specs = (
        P(None, "sp", "tp"),
        P(),
        P(None, "sp", "tp"),
        P(None, "sp", "tp"),
        P(None, "sp", "tp"),
        P(None, None, "tp"),
        P(None, "sp", "tp"),
    )
    out_specs = P(None, "sp", "tp")
    return jax.shard_map(body, mesh=mesh, in_specs=in_specs, out_specs=out_specs, check_vma=False)
```

```python
import functools

import jax
import jax.numpy as jnp
from jax import lax
from jax.experimental import pallas as pl
from jax.experimental.pallas import tpu as pltpu
from jax.sharding import PartitionSpec as P

MESH = pl.DeviceIdType.MESH
EPS = 1e-06
L = 3
HALO = 16
ROWS_A, ROWS_B = 256, 128
A0 = HALO
B0 = HALO + ROWS_A + HALO
ROWS = B0 + ROWS_B
BF, F32 = jnp.bfloat16, jnp.float32

ORDERS = (
    ("xyz", "xyz", "xyz"),
    ("yzx", "yzx", "yzx"),
    ("zxy", "zxy", "zxy"),
    ("xyz", "xyz", "xyz"),
    ("xzy", "xzy", "xzy"),
)
NMAT = 5
EVERY, PROJ, OUTP = (0, 1, 2, 3, 4), (0, 1, 2), (3, 4)


class Sems:
    def __init__(self):
        self.at = {}

    def __getitem__(self, key):
        return self.at.setdefault(key, len(self.at))


N_SEMS = 288


def kernel(
    tokens, gains, w_o, w_i, w_v, taps, w_u, out, wx, wu, x_buf, n_buf, m_buf, g_buf, t_buf, send, recv, local
):
    sp, x = lax.axis_index("sp"), lax.axis_index("tp")
    c, y, z = lax.rem(sp, 2), lax.rem(sp // 2, 4), sp // 8
    sems = Sems()
    pending = []
    args = (w_o, w_i, w_v, w_u.at[:, pl.ds(0, 16)], w_u.at[:, pl.ds(16, 16)])

    def device(dx=0, dy=0, dz=0, dc=0):
        sp_of = lax.rem(z + dz + 4, 4) * 8 + lax.rem(y + dy + 4, 4) * 2 + lax.rem(c + dc, 2)
        return (sp_of, lax.rem(x + dx + 4, 4))

    def neighbour(dim, sign):
        return device(**{"d" + dim: sign})

    def remote(src, dst, key, dev):
        k = sems[key]
        return pltpu.make_async_remote_copy(
            src_ref=src, dst_ref=dst, send_sem=send.at[k], recv_sem=recv.at[k], device_id=dev, device_id_type=MESH
        )

    def start(src, dst, key, dev):
        copy = remote(src, dst, key, dev)
        copy.start()
        pending.append(copy)

    def arrived(dst, key):
        remote(dst, dst, key, device(dc=1)).wait_recv()

    def region(m, layer, full, moved=None, by=0, half=None, core=None):
        place = {"x": x, "y": y, "z": z}
        core = c if core is None else core
        if moved is not None:
            place[moved] = lax.rem(place[moved] + by + 4, 4)
        pick = [slice(None) if d in full else place[d] for d in "xzy"]
        if m < 3:
            tail = slice(None) if half is None else pl.ds(half * 32, 32)
        else:
            tail = pl.ds(16 * (m - 3), 16) if half is None else pl.ds(16 * (m - 3) + 8 * half, 8)
        if m < 3:
            return wx.at[(layer, m, *pick, core, tail)]
        return wu.at[(layer, *pick, core, tail)]

    ALL = slice(None)

    barrier = pltpu.get_barrier_semaphore()
    left_sp, right_sp = lax.rem(sp + 31, 32), lax.rem(sp + 1, 32)
    peers = [device(dx=d) for d in (1, 2, 3)]
    peers += [neighbour(d, s) for d in "yz" for s in (1, -1)]
    peers.append(device(dc=1))
    for d in range(4):
        peers += [(right_sp, lax.rem(x + d, 4)), (left_sp, lax.rem(x + d, 4))]
    for peer in peers:
        pl.semaphore_signal(barrier, inc=1, device_id=peer, device_id_type=MESH)
    g_buf[pl.ds(0, 8), :] = jnp.zeros((8, 256), F32)
    own = []
    for m in range(NMAT):
        own.append(pltpu.make_async_copy(args[m], region(m, ALL, ""), local.at[m]))
        own[-1].start()
    pl.semaphore_wait(barrier, len(peers))

    for m in range(NMAT):
        d = ORDERS[m][0][0]
        for s in (1, -1):
            start(args[m], region(m, ALL, ""), (m, 1, s), neighbour(d, s))

    def rows_of(xd):
        return 3 * (xd // 2) + 2 * lax.rem(xd, 2), 3 * (xd // 2) + 1, lax.rem(xd, 2)

    def token_copies():
        found = []
        for d in range(4):
            xd = lax.rem(x + d, 4)
            seq_a, seq_b, odd = rows_of(xd)
            row_b = pl.multiple_of(128 * odd, 128)
            here = (sp, xd)
            there = (right_sp, xd)
            pieces = [
                (None, tokens.at[seq_a], x_buf.at[x, pl.ds(A0, ROWS_A)], "a", here),
                (None, tokens.at[seq_b, pl.ds(row_b, ROWS_B)], x_buf.at[x, pl.ds(B0, ROWS_B)], "b", here),
                (sp < 31, tokens.at[seq_a, pl.ds(240, 16)], x_buf.at[x, pl.ds(0, 16)], "ha", there),
                ((odd == 0) & (sp < 31), tokens.at[seq_b, pl.ds(240, 16)], x_buf.at[x, pl.ds(B0 - 16, 16)], "he", there),
                (odd == 1, tokens.at[seq_b, pl.ds(112, 16)], x_buf.at[x, pl.ds(B0 - 16, 16)], "ho", here),
            ]
            for when, src, dst, name, dev in pieces:
                key = ("tok", name, d)
                if d == 0 and name in ("a", "b", "ho"):
                    copy = pltpu.make_async_copy(src, dst, local.at[{"a": 5, "b": 6, "ho": 7}[name]])
                    found.append((when, copy, True))
                else:
                    found.append((when, remote(src, dst, key, dev), False))
        return found

    def guarded(when, action):
        if when is None:
            action()
        else:
            pl.when(when)(action)

    pltpu.make_async_copy(taps, t_buf.at[x], local.at[8]).start()
    for d in (1, 2, 3):
        start(taps, t_buf.at[x], ("taps", d), device(dx=d))
    token_list = token_copies()

    def start_tokens():
        for when, copy, _ in token_list:
            guarded(when, copy.start)

    def wait_tokens():
        for when, copy, is_local in token_list:
            if is_local:
                guarded(when, copy.wait)
        odd = lax.rem(x, 2)
        for d in range(4):
            xs = lax.rem(x - d + 4, 4)
            arriving = [
                (None, x_buf.at[xs, pl.ds(A0, ROWS_A)], "a"),
                (None, x_buf.at[xs, pl.ds(B0, ROWS_B)], "b"),
                (sp > 0, x_buf.at[xs, pl.ds(0, 16)], "ha"),
                ((odd == 0) & (sp > 0), x_buf.at[xs, pl.ds(B0 - 16, 16)], "he"),
                (odd == 1, x_buf.at[xs, pl.ds(B0 - 16, 16)], "ho"),
            ]
            for when, dst, name in arriving:
                if d == 0 and name in ("a", "b", "ho"):
                    continue
                guarded(when, functools.partial(arrived, dst, ("tok", name, d)))

        @pl.when(sp == 0)
        def _():
            x_buf[:, pl.ds(0, 16), :] = jnp.zeros((4, 16, 512), BF)

        @pl.when((sp == 0) & (odd == 0))
        def _():
            x_buf[:, pl.ds(B0 - 16, 16), :] = jnp.zeros((4, 16, 512), BF)

        pltpu.make_async_copy(taps, t_buf.at[x], local.at[8]).wait()
        for d in (1, 2, 3):
            arrived(t_buf.at[lax.rem(x - d + 4, 4)], ("taps", d))

    for m in range(NMAT):
        d = ORDERS[m][0][0]
        for s in (1, -1):
            arrived(region(m, ALL, "", d, -s), (m, 1, s))
            part = region(m, ALL, "", d, -s, half=0 if s == 1 else 1)
            start(part, part, (m, 2, s), neighbour(d, s))
    for m in range(NMAT):
        own[m].wait()

    for layer in range(L):
        for m in range(NMAT):
            first, d, _ = ORDERS[m][layer]
            if layer == 0:
                for s in (1, -1):
                    arrived(region(m, ALL, "", first, -2 * s, half=0 if s == 1 else 1), (m, 2, s))
            for s in (1, -1):
                block = region(m, layer, first)
                start(block, block, (m, layer, 3, s), neighbour(d, s))
    for layer in range(L):
        for m in range(NMAT):
            first, d, _ = ORDERS[m][layer]
            for s in (1, -1):
                arrived(region(m, layer, first, d, -s), (m, layer, 3, s))
                part = region(m, layer, first, d, -s, half=0 if s == 1 else 1)
                start(part, part, (m, layer, 4, s), neighbour(d, s))

    partner = device(dc=1)

    def second_done(layer):
        for m in range(NMAT):
            first, d, _ = ORDERS[m][layer]
            for s in (1, -1):
                arrived(region(m, layer, first, d, -2 * s, half=0 if s == 1 else 1), (m, layer, 4, s))

    def third(layer, part, mats=EVERY):
        for m in mats:
            first, second, d = ORDERS[m][layer]
            for s in (1, -1):
                half = part if s == 1 else 1 - part
                block = region(m, layer, first + second, half=half)
                start(block, block, (m, layer, 5 + part, s), neighbour(d, s))

    def across(m, layer, which, half=None):
        first, second, d = ORDERS[m][layer]
        block = region(m, layer, first + second, d, which, half)
        start(block, block, (m, layer, "core", which, half), partner)

    def own_across(layer):
        for m in EVERY:
            across(m, layer, 0)

    def pass_on(layer, mats=EVERY):
        for m in mats:
            first, second, d = ORDERS[m][layer]
            for s in (1, -1):
                part = region(m, layer, first + second, d, -s, half=0 if s == 1 else 1)
                arrived(part, (m, layer, 5, s))
                start(part, part, (m, layer, 7, s), neighbour(d, s))

    def near_done(layer, mats=EVERY):
        for m in mats:
            first, second, d = ORDERS[m][layer]
            for s in (1, -1):
                arrived(region(m, layer, first + second, d, -s, half=1 if s == 1 else 0), (m, layer, 6, s))
                across(m, layer, -s)

    def far_done(layer, mats=EVERY):
        for m in mats:
            first, second, d = ORDERS[m][layer]
            for s in (1, -1):
                half = 0 if s == 1 else 1
                arrived(region(m, layer, first + second, d, 2, half=half), (m, layer, 7, s))
                across(m, layer, 2, half)

    def from_partner(layer, mats=EVERY):
        for which, half in ((0, None), (1, None), (-1, None), (2, 0), (2, 1)):
            for m in mats:
                first, second, d = ORDERS[m][layer]
                block = region(m, layer, first + second, d, which, half, core=1 - c)
                arrived(block, (m, layer, "core", which, half))

    def normalize(layer):
        def step(r, _):
            rows = pl.ds(pl.multiple_of(r * 32, 32), 32)
            total = jnp.zeros((32, 1), F32)
            for k in range(4):
                v = x_buf[k, rows, :].astype(F32)
                total += jnp.sum(v * v, axis=-1, keepdims=True)
            scale = lax.rsqrt(total * (1.0 / 2048) + EPS)
            for k in range(4):
                v = x_buf[k, rows, :].astype(F32)
                gain = gains[pl.ds(layer, 1), pl.ds(k * 512, 512)]
                n_buf[rows, pl.ds(k * 512, 512)] = (v * scale * gain).astype(BF)
            return 0

        lax.fori_loop(0, ROWS // 32, step, 0)

    def mix(layer, begin=0, end=4):
        def step(b, _):
            def project(m):
                weight = wx[layer, m, b].reshape(2048, 256)
                return jnp.dot(n_buf[...], weight, preferred_element_type=F32).astype(BF).astype(F32)

            g_buf[pl.ds(8, ROWS), :] = project(1) * project(2)
            outer = project(0)
            conved = jnp.zeros((ROWS, 256), F32)
            for k in range(3):
                conved += t_buf[b, layer, pl.ds(k, 1), :] * g_buf[pl.ds(6 + k, ROWS), :]
            m_buf[:, pl.ds(pl.multiple_of(b * 256, 256), 256)] = (outer * conved).astype(BF)
            return 0

        lax.fori_loop(begin, end, step, 0)

    def project_out(layer, b):
        weight = wu[layer, b].reshape(1024, 512)
        x_buf[b] = jnp.dot(m_buf[...], weight, preferred_element_type=F32).astype(BF)

    def project_all(layer):
        def step(b, _):
            project_out(layer, b)
            return 0

        lax.fori_loop(0, 4, step, 0)

    second_done(0)
    third(0, 0)
    third(0, 1)
    own_across(0)
    second_done(1)
    third(1, 0)
    own_across(1)
    start_tokens()
    second_done(2)
    own_across(2)
    pass_on(0)
    third(1, 1)
    third(2, 0, PROJ)
    near_done(0)
    far_done(0)
    wait_tokens()
    normalize(0)
    from_partner(0)
    mix(0)
    project_all(0)
    pass_on(1)
    third(2, 1, PROJ)
    third(2, 0, OUTP)
    normalize(1)
    near_done(1)
    far_done(1)
    from_partner(1)
    mix(1)
    project_all(1)
    pass_on(2, PROJ)
    third(2, 1, OUTP)
    normalize(2)
    pass_on(2, OUTP)
    near_done(2, PROJ)
    far_done(2, PROJ)
    from_partner(2, PROJ)
    mix(2, 0, 2)
    near_done(2, OUTP)
    mix(2, 2, 3)
    far_done(2, OUTP)
    mix(2, 3, 4)
    from_partner(2, OUTP)

    seq_a, seq_b, odd = rows_of(x)
    row_b = pl.multiple_of(128 * odd, 128)
    dst_a = out.at[seq_a]
    dst_b = out.at[seq_b, pl.ds(row_b, ROWS_B)]
    for d in (2, 1, 3, 0):
        xd = lax.rem(x + d, 4)
        project_out(L - 1, xd)
        src_a, src_b = x_buf.at[xd, pl.ds(A0, ROWS_A)], x_buf.at[xd, pl.ds(B0, ROWS_B)]
        if d == 0:
            last = [pltpu.make_async_copy(src_a, dst_a, local.at[5]), pltpu.make_async_copy(src_b, dst_b, local.at[6])]
            for copy in last:
                copy.start()
        else:
            start(src_a, dst_a, ("out", "a", d), (sp, xd))
            start(src_b, dst_b, ("out", "b", d), (sp, xd))
    for when, copy, is_local in token_list:
        if not is_local:
            guarded(when, copy.wait_send)
    for copy in pending:
        copy.wait_send()
    for d in (2, 1, 3):
        from_a, from_b, from_odd = rows_of(lax.rem(x - d + 4, 4))
        arrived(out.at[from_a], ("out", "a", d))
        arrived(out.at[from_b, pl.ds(pl.multiple_of(128 * from_odd, 128), ROWS_B)], ("out", "b", d))
    for copy in last:
        copy.wait()
    assert len(sems.at) <= N_SEMS


def body(tokens, norm_gains, weight_outer, weight_inner, weight_value, conv_taps, weight_output):
    taps = jnp.pad(conv_taps.astype(F32), ((0, 0), (0, 5), (0, 0)))
    hbm = pl.BlockSpec(memory_space=pl.ANY)
    vmem = pl.BlockSpec(memory_space=pltpu.VMEM)
    result = pl.pallas_call(
        kernel,
        out_shape=jax.ShapeDtypeStruct((6, 256, 512), BF),
        in_specs=[hbm, vmem, hbm, hbm, hbm, hbm, hbm],
        out_specs=hbm,
        scratch_shapes=[
            pltpu.VMEM((L, 3, 4, 4, 4, 2, 64, 256), BF),
            pltpu.VMEM((L, 4, 4, 4, 2, 32, 512), BF),
            pltpu.VMEM((4, ROWS, 512), BF),
            pltpu.VMEM((ROWS, 2048), BF),
            pltpu.VMEM((ROWS, 1024), BF),
            pltpu.VMEM((ROWS + 8, 256), F32),
            pltpu.VMEM((4, 3, 8, 256), F32),
            pltpu.SemaphoreType.DMA((N_SEMS,)),
            pltpu.SemaphoreType.DMA((N_SEMS,)),
            pltpu.SemaphoreType.DMA((9,)),
        ],
        compiler_params=pltpu.CompilerParams(
            collective_id=0, has_side_effects=True, vmem_limit_bytes=67_000_000
        ),
        name="mixers",
    )(tokens, norm_gains, weight_outer, weight_inner, weight_value, taps, weight_output)
    return result.astype(F32)


def solution(mesh):
    in_specs = (
        P(None, "sp", "tp"),
        P(),
        P(None, "sp", "tp"),
        P(None, "sp", "tp"),
        P(None, "sp", "tp"),
        P(None, None, "tp"),
        P(None, "sp", "tp"),
    )
    out_specs = P(None, "sp", "tp")
    return jax.shard_map(body, mesh=mesh, in_specs=in_specs, out_specs=out_specs, check_vma=False)
```

```python
import functools

import jax
import jax.numpy as jnp
from jax import lax
from jax.experimental import pallas as pl
from jax.experimental.pallas import tpu as pltpu
from jax.sharding import PartitionSpec as P

MESH = pl.DeviceIdType.MESH
EPS = 1e-06
L = 3
HALO = 16
ROWS_A, ROWS_B = 256, 128
A0 = HALO
B0 = HALO + ROWS_A + HALO
ROWS = B0 + ROWS_B
BF, F32 = jnp.bfloat16, jnp.float32

ORDERS = (
    "xyz",
    "yzx",
    "zxy",
    "xyz",
    "xzy",
)
NMAT = 5
EVERY, PROJ, OUTP = (0, 1, 2, 3, 4), (0, 1, 2), (3, 4)
ON_X, ON_YZ = (1,), (0, 2, 3, 4)


class Sems:
    def __init__(self):
        self.at = {}

    def __getitem__(self, key):
        return self.at.setdefault(key, len(self.at))


N_SEMS = 296


def kernel(
    tokens, gains, w_o, w_i, w_v, taps, w_u, out, wx, wu, x_buf, n_buf, m_buf, g_buf, t_buf, send, recv, local
):
    sp, x = lax.axis_index("sp"), lax.axis_index("tp")
    c, y, z = lax.rem(sp, 2), lax.rem(sp // 2, 4), sp // 8
    sems = Sems()
    pending = []
    args = (w_o, w_i, w_v, w_u.at[:, pl.ds(0, 16)], w_u.at[:, pl.ds(16, 16)])

    def device(dx=0, dy=0, dz=0, dc=0):
        sp_of = lax.rem(z + dz + 4, 4) * 8 + lax.rem(y + dy + 4, 4) * 2 + lax.rem(c + dc, 2)
        return (sp_of, lax.rem(x + dx + 4, 4))

    def neighbour(dim, sign):
        return device(**{"d" + dim: sign})

    def remote(src, dst, key, dev):
        k = sems[key]
        return pltpu.make_async_remote_copy(
            src_ref=src, dst_ref=dst, send_sem=send.at[k], recv_sem=recv.at[k], device_id=dev, device_id_type=MESH
        )

    def start(src, dst, key, dev):
        copy = remote(src, dst, key, dev)
        copy.start()
        pending.append(copy)

    def arrived(dst, key):
        remote(dst, dst, key, device(dc=1)).wait_recv()

    def region(m, layer, full, moved=None, half=None, core=None):
        place = {"x": x, "y": y, "z": z}
        core = c if core is None else core
        for dim, step in (moved or {}).items():
            place[dim] = lax.rem(place[dim] + step + 4, 4)
        pick = [slice(None) if d in full else place[d] for d in "xzy"]
        if m < 3:
            tail = slice(None) if half is None else pl.ds(half * 32, 32)
        else:
            tail = pl.ds(16 * (m - 3), 16) if half is None else pl.ds(16 * (m - 3) + 8 * half, 8)
        if m < 3:
            return wx.at[(layer, m, *pick, core, tail)]
        return wu.at[(layer, *pick, core, tail)]

    ALL = slice(None)

    barrier = pltpu.get_barrier_semaphore()
    left_sp, right_sp = lax.rem(sp + 31, 32), lax.rem(sp + 1, 32)
    peers = [device(dx=d) for d in (1, 2, 3)]
    peers += [neighbour(d, s) for d in "yz" for s in (1, -1)]
    peers.append(device(dc=1))
    for d in range(4):
        peers += [(right_sp, lax.rem(x + d, 4)), (left_sp, lax.rem(x + d, 4))]
    for peer in peers:
        pl.semaphore_signal(barrier, inc=1, device_id=peer, device_id_type=MESH)
    g_buf[pl.ds(0, 8), :] = jnp.zeros((8, 256), F32)
    own = []
    for m in range(NMAT):
        own.append(pltpu.make_async_copy(args[m], region(m, ALL, ""), local.at[m]))
        own[-1].start()
    pl.semaphore_wait(barrier, len(peers))

    for m in range(NMAT):
        for s in (1, -1):
            start(args[m], region(m, ALL, ""), (m, 1, s), neighbour(ORDERS[m][0], s))
    for m in range(NMAT):
        for s in (1, -1):
            start(args[m], region(m, ALL, ""), (m, 3, s, 0), neighbour(ORDERS[m][1], s))

    def rows_of(xd):
        return 3 * (xd // 2) + 2 * lax.rem(xd, 2), 3 * (xd // 2) + 1, lax.rem(xd, 2)

    def token_copies():
        found = []
        for d in range(4):
            xd = lax.rem(x + d, 4)
            seq_a, seq_b, odd = rows_of(xd)
            row_b = pl.multiple_of(128 * odd, 128)
            here = (sp, xd)
            there = (right_sp, xd)
            pieces = [
                (None, tokens.at[seq_a], x_buf.at[x, pl.ds(A0, ROWS_A)], "a", here),
                (None, tokens.at[seq_b, pl.ds(row_b, ROWS_B)], x_buf.at[x, pl.ds(B0, ROWS_B)], "b", here),
                (sp < 31, tokens.at[seq_a, pl.ds(240, 16)], x_buf.at[x, pl.ds(0, 16)], "ha", there),
                ((odd == 0) & (sp < 31), tokens.at[seq_b, pl.ds(240, 16)], x_buf.at[x, pl.ds(B0 - 16, 16)], "he", there),
                (odd == 1, tokens.at[seq_b, pl.ds(112, 16)], x_buf.at[x, pl.ds(B0 - 16, 16)], "ho", here),
            ]
            for when, src, dst, name, dev in pieces:
                key = ("tok", name, d)
                if d == 0 and name in ("a", "b", "ho"):
                    copy = pltpu.make_async_copy(src, dst, local.at[{"a": 5, "b": 6, "ho": 7}[name]])
                    found.append((when, copy, True))
                else:
                    found.append((when, remote(src, dst, key, dev), False))
        return found

    def guarded(when, action):
        if when is None:
            action()
        else:
            pl.when(when)(action)

    t_buf[x] = taps[...]
    for d in (1, 2, 3):
        start(taps, t_buf.at[x], ("taps", d), device(dx=d))
    token_list = token_copies()

    def start_tokens():
        for when, copy, _ in token_list:
            guarded(when, copy.start)

    def wait_tokens():
        for when, copy, is_local in token_list:
            if is_local:
                guarded(when, copy.wait)
        odd = lax.rem(x, 2)
        for d in range(4):
            xs = lax.rem(x - d + 4, 4)
            arriving = [
                (None, x_buf.at[xs, pl.ds(A0, ROWS_A)], "a"),
                (None, x_buf.at[xs, pl.ds(B0, ROWS_B)], "b"),
                (sp > 0, x_buf.at[xs, pl.ds(0, 16)], "ha"),
                ((odd == 0) & (sp > 0), x_buf.at[xs, pl.ds(B0 - 16, 16)], "he"),
                (odd == 1, x_buf.at[xs, pl.ds(B0 - 16, 16)], "ho"),
            ]
            for when, dst, name in arriving:
                if d == 0 and name in ("a", "b", "ho"):
                    continue
                guarded(when, functools.partial(arrived, dst, ("tok", name, d)))

        @pl.when(sp == 0)
        def _():
            x_buf[:, pl.ds(0, 16), :] = jnp.zeros((4, 16, 512), BF)

        @pl.when((sp == 0) & (odd == 0))
        def _():
            x_buf[:, pl.ds(B0 - 16, 16), :] = jnp.zeros((4, 16, 512), BF)

        for d in (1, 2, 3):
            arrived(t_buf.at[lax.rem(x - d + 4, 4)], ("taps", d))

    def spread(m, by):
        for s in (1, -1):
            block = region(m, ALL, "", {ORDERS[m][0]: by})
            start(block, block, (m, 3, s, by), neighbour(ORDERS[m][1], s))

    for m in range(NMAT):
        d = ORDERS[m][0]
        for s in (1, -1):
            arrived(region(m, ALL, "", {d: -s}), (m, 1, s))
            part = region(m, ALL, "", {d: -s}, half=0 if s == 1 else 1)
            start(part, part, (m, 2, s), neighbour(d, s))
    for m in range(NMAT):
        spread(m, -1)
        spread(m, 1)
    for m in range(NMAT):
        own[m].wait()
        for s in (1, -1):
            arrived(region(m, ALL, "", {ORDERS[m][0]: 2}, half=0 if s == 1 else 1), (m, 2, s))
        spread(m, 2)

    for layer in range(L):
        for m in range(NMAT):
            first, d, _ = ORDERS[m]
            for s in (1, -1):
                if layer == 0:
                    for by in (0, -1, 1, 2):
                        arrived(region(m, ALL, "", {first: by, d: -s}), (m, 3, s, by))
                part = region(m, layer, first, {d: -s}, half=0 if s == 1 else 1)
                start(part, part, (m, layer, 4, s), neighbour(d, s))

    partner = device(dc=1)

    def second_done(layer):
        for m in range(NMAT):
            first, d, _ = ORDERS[m]
            for s in (1, -1):
                arrived(region(m, layer, first, {d: 2}, half=0 if s == 1 else 1), (m, layer, 4, s))

    def third(layer, part, mats=EVERY):
        for m in mats:
            first, second, d = ORDERS[m]
            for s in (1, -1):
                half = part if s == 1 else 1 - part
                block = region(m, layer, first + second, half=half)
                start(block, block, (m, layer, 5 + part, s), neighbour(d, s))

    def across(m, layer, which, half=None):
        first, second, d = ORDERS[m]
        block = region(m, layer, first + second, {d: which}, half)
        start(block, block, (m, layer, "core", which, half), partner)

    def own_across(layer):
        for m in EVERY:
            across(m, layer, 0)

    def pass_on(layer, mats=EVERY):
        for m in mats:
            first, second, d = ORDERS[m]
            for s in (1, -1):
                part = region(m, layer, first + second, {d: -s}, half=0 if s == 1 else 1)
                arrived(part, (m, layer, 5, s))
                start(part, part, (m, layer, 7, s), neighbour(d, s))

    def near_done(layer, mats=EVERY):
        for m in mats:
            first, second, d = ORDERS[m]
            for s in (1, -1):
                arrived(region(m, layer, first + second, {d: -s}, half=1 if s == 1 else 0), (m, layer, 6, s))
                across(m, layer, -s)

    def far_done(layer, mats=EVERY):
        for m in mats:
            first, second, d = ORDERS[m]
            for s in (1, -1):
                half = 0 if s == 1 else 1
                arrived(region(m, layer, first + second, {d: 2}, half=half), (m, layer, 7, s))
                across(m, layer, 2, half)

    def from_partner(layer, mats=EVERY):
        for which, half in ((0, None), (1, None), (-1, None), (2, 0), (2, 1)):
            for m in mats:
                first, second, d = ORDERS[m]
                block = region(m, layer, first + second, {d: which}, half, core=1 - c)
                arrived(block, (m, layer, "core", which, half))

    def normalize(layer):
        def step(r, _):
            rows = pl.ds(pl.multiple_of(r * 32, 32), 32)
            total = jnp.zeros((32, 1), F32)
            for k in range(4):
                v = x_buf[k, rows, :].astype(F32)
                total += jnp.sum(v * v, axis=-1, keepdims=True)
            scale = lax.rsqrt(total * (1.0 / 2048) + EPS)
            for k in range(4):
                v = x_buf[k, rows, :].astype(F32)
                gain = gains[pl.ds(layer, 1), pl.ds(k * 512, 512)]
                n_buf[rows, pl.ds(k * 512, 512)] = (v * scale * gain).astype(BF)
            return 0

        lax.fori_loop(0, ROWS // 32, step, 0)

    def mix(layer, begin=0, end=4):
        def step(b, _):
            def project(m):
                weight = wx[layer, m, b].reshape(2048, 256)
                return jnp.dot(n_buf[...], weight, preferred_element_type=F32).astype(BF).astype(F32)

            g_buf[pl.ds(8, ROWS), :] = project(1) * project(2)
            outer = project(0)
            tap = t_buf[b, layer].astype(F32)
            conved = jnp.zeros((ROWS, 256), F32)
            for k in range(3):
                conved += tap[k : k + 1, :] * g_buf[pl.ds(6 + k, ROWS), :]
            m_buf[:, pl.ds(pl.multiple_of(b * 256, 256), 256)] = (outer * conved).astype(BF)
            return 0

        lax.fori_loop(begin, end, step, 0)

    def project_out(layer, b):
        weight = wu[layer, b].reshape(1024, 512)
        x_buf[b] = jnp.dot(m_buf[...], weight, preferred_element_type=F32).astype(BF)

    def project_all(layer):
        def step(b, _):
            project_out(layer, b)
            return 0

        lax.fori_loop(0, 4, step, 0)

    start_tokens()
    second_done(0)
    third(0, 0)
    third(0, 1)
    own_across(0)
    second_done(1)
    own_across(1)
    second_done(2)
    own_across(2)
    pass_on(0, ON_YZ)
    third(1, 0, ON_YZ)
    third(1, 1, ON_YZ)
    wait_tokens()
    normalize(0)
    near_done(0, ON_YZ)
    pass_on(0, ON_X)
    third(1, 0, ON_X)
    third(1, 1, ON_X)
    near_done(0, ON_X)
    far_done(0, ON_YZ)
    far_done(0, ON_X)
    from_partner(0)
    mix(0, 0, 2)
    pass_on(1, ON_X)
    third(2, 0, ON_X)
    third(2, 1, ON_X)
    pass_on(1, ON_YZ)
    third(2, 0, (0, 2))
    third(2, 1, (0, 2))
    third(2, 0, OUTP)
    mix(0, 2, 4)
    near_done(1, ON_X)
    project_all(0)
    near_done(1, ON_YZ)
    normalize(1)
    far_done(1, ON_X)
    far_done(1, ON_YZ)
    from_partner(1)
    mix(1, 0, 2)
    pass_on(2, PROJ)
    third(2, 1, OUTP)
    mix(1, 2, 4)
    near_done(2, PROJ)
    project_all(1)
    pass_on(2, OUTP)
    normalize(2)
    far_done(2, PROJ)
    from_partner(2, PROJ)
    mix(2, 0, 2)
    near_done(2, OUTP)
    mix(2, 2, 3)
    far_done(2, OUTP)
    mix(2, 3, 4)
    from_partner(2, OUTP)

    seq_a, seq_b, odd = rows_of(x)
    row_b = pl.multiple_of(128 * odd, 128)
    dst_a = out.at[seq_a]
    dst_b = out.at[seq_b, pl.ds(row_b, ROWS_B)]
    for d in (2, 1, 3, 0):
        xd = lax.rem(x + d, 4)
        project_out(L - 1, xd)
        src_a, src_b = x_buf.at[xd, pl.ds(A0, ROWS_A)], x_buf.at[xd, pl.ds(B0, ROWS_B)]
        if d == 0:
            last = [pltpu.make_async_copy(src_a, dst_a, local.at[5]), pltpu.make_async_copy(src_b, dst_b, local.at[6])]
            for copy in last:
                copy.start()
        else:
            start(src_a, dst_a, ("out", "a", d), (sp, xd))
            start(src_b, dst_b, ("out", "b", d), (sp, xd))
    for when, copy, is_local in token_list:
        if not is_local:
            guarded(when, copy.wait_send)
    for copy in pending:
        copy.wait_send()
    for d in (2, 1, 3):
        from_a, from_b, from_odd = rows_of(lax.rem(x - d + 4, 4))
        arrived(out.at[from_a], ("out", "a", d))
        arrived(out.at[from_b, pl.ds(pl.multiple_of(128 * from_odd, 128), ROWS_B)], ("out", "b", d))
    for copy in last:
        copy.wait()
    assert len(sems.at) <= N_SEMS


def body(tokens, norm_gains, weight_outer, weight_inner, weight_value, conv_taps, weight_output):
    hbm = pl.BlockSpec(memory_space=pl.ANY)
    vmem = pl.BlockSpec(memory_space=pltpu.VMEM)
    result = pl.pallas_call(
        kernel,
        out_shape=jax.ShapeDtypeStruct((6, 256, 512), BF),
        in_specs=[hbm, vmem, hbm, hbm, hbm, vmem, hbm],
        out_specs=hbm,
        scratch_shapes=[
            pltpu.VMEM((L, 3, 4, 4, 4, 2, 64, 256), BF),
            pltpu.VMEM((L, 4, 4, 4, 2, 32, 512), BF),
            pltpu.VMEM((4, ROWS, 512), BF),
            pltpu.VMEM((ROWS, 2048), BF),
            pltpu.VMEM((ROWS, 1024), BF),
            pltpu.VMEM((ROWS + 8, 256), F32),
            pltpu.VMEM((4, 3, 3, 256), BF),
            pltpu.SemaphoreType.DMA((N_SEMS,)),
            pltpu.SemaphoreType.DMA((N_SEMS,)),
            pltpu.SemaphoreType.DMA((8,)),
        ],
        compiler_params=pltpu.CompilerParams(
            collective_id=0, has_side_effects=True, vmem_limit_bytes=67_000_000
        ),
        name="mixers",
    )(tokens, norm_gains, weight_outer, weight_inner, weight_value, conv_taps, weight_output)
    return result.astype(F32)


def solution(mesh):
    in_specs = (
        P(None, "sp", "tp"),
        P(),
        P(None, "sp", "tp"),
        P(None, "sp", "tp"),
        P(None, "sp", "tp"),
        P(None, None, "tp"),
        P(None, "sp", "tp"),
    )
    out_specs = P(None, "sp", "tp")
    return jax.shard_map(body, mesh=mesh, in_specs=in_specs, out_specs=out_specs, check_vma=False)
```

```python
import functools

import jax
import jax.numpy as jnp
from jax import lax
from jax.experimental import pallas as pl
from jax.experimental.pallas import tpu as pltpu
from jax.sharding import PartitionSpec as P

MESH = pl.DeviceIdType.MESH
EPS = 1e-06
L = 3
HALO = 16
ROWS_A, ROWS_B = 256, 128
A0 = HALO
B0 = HALO + ROWS_A + HALO
ROWS = B0 + ROWS_B
BF, F32 = jnp.bfloat16, jnp.float32

FIRST_ORDERS = ("zyx", "yxz", "xzy")
OUTPUT_ORDERS = ("xyz", "xzy")
COLUMN_ORDERS = (("yz", "zy", "yz"), ("zy", "zy", "zy"))
FOLDED_ORDERS = (("yzx", "yxz", "zyx"), ("yxz", "zyx", "zxy"))


class Sems:
    def __init__(self):
        self.at = {}

    def __getitem__(self, key):
        return self.at.setdefault(key, len(self.at))


N_RECV, N_SEND = 168, 40


def kernel(
    tokens, gains, w_o, w_i, w_v, taps, w_u, out,
    wx, wu, wf, wp, x_buf, n_buf, m_buf, g_buf, t_buf, h_buf, p_buf, s_buf, send, recv, local,
):
    sp, x = lax.axis_index("sp"), lax.axis_index("tp")
    c, y, z = lax.rem(sp, 2), lax.rem(sp // 2, 4), sp // 8
    sems, sent = Sems(), Sems()
    args = (w_o, w_i, w_v)

    def device(dx=0, dy=0, dz=0, dc=0):
        sp_of = lax.rem(z + dz + 4, 4) * 8 + lax.rem(y + dy + 4, 4) * 2 + lax.rem(c + dc, 2)
        return (sp_of, lax.rem(x + dx + 4, 4))

    def neighbour(dim, sign):
        return device(**{"d" + dim: sign})

    def remote(src, dst, group, key, dev):
        return pltpu.make_async_remote_copy(
            src_ref=src,
            dst_ref=dst,
            send_sem=send.at[sent[group]],
            recv_sem=recv.at[sems[key]],
            device_id=dev,
            device_id_type=MESH,
        )

    def start(src, dst, group, key, dev):
        remote(src, dst, group, key, dev).start()

    def arrived(dst, key):
        remote(dst, dst, "any", key, device(dc=1)).wait_recv()

    def all_sent(src, group):
        remote(src, src, group, "any", device(dc=1)).wait_send()

    ALL = slice(None)
    partner = device(dc=1)

    class Ring:
        def __init__(self, kind, key, order, ref, rows):
            self.kind, self.key, self.order, self.ref, self.rows = kind, key, order, ref, rows

        def part(self, full="", moved=None, half=None, core=None, span=None):
            place = {"x": x, "y": y, "z": z}
            for dim, step in (moved or {}).items():
                place[dim] = lax.rem(place[dim] + step + 4, 4)
            place.update({d: ALL for d in full})
            place.update(span or {})
            first, rows = self.rows
            tail = pl.ds(first, rows) if half is None else pl.ds(first + half * (rows // 2), rows // 2)
            return self.ref(place, c if core is None else core, tail)

        def send(self, src, step, dim, sign, stage):
            start(src, src, (self.kind, stage), (self.key, step), neighbour(dim, sign))

        def one(self):
            for s in (1, -1):
                self.send(self.part(), 1, self.order[0], s, 1)

        def own_two(self):
            for s in (1, -1):
                self.send(self.part(), 3, self.order[1], s, 2)

        def spread(self, by):
            for s in (1, -1):
                self.send(self.part(moved={self.order[0]: by}), 3, self.order[1], s, 2)

        def one_on(self, spread=True):
            d = self.order[0]
            arrived(self.part(span={d: pl.ds(0, 2)}), (self.key, 1))
            for s in (1, -1):
                self.send(self.part(moved={d: -s}, half=0 if s == 1 else 1), 2, d, s, 1)
            if spread:
                self.spread(-1)
                self.spread(1)

        def one_done(self, spread=True):
            arrived(self.part(), (self.key, 2))
            if spread:
                self.spread(2)

        def two_all(self):
            self.own_two()
            for by in (-1, 1, 2):
                self.spread(by)

        def two_on(self):
            first, d = self.order[:2]
            arrived(self.part(first, span={d: pl.ds(0, 2)}), (self.key, 3))
            for s in (1, -1):
                self.send(self.part(first, {d: -s}, 0 if s == 1 else 1), 4, d, s, 3)
            if len(self.order) == 2:
                for which in (0, 1, -1):
                    self.across(which)

        def two_done(self):
            arrived(self.part(self.order[0]), (self.key, 4))
            self.across(2 if len(self.order) == 2 else 0)

        def three(self, which):
            for s in (1, -1):
                half = which if s == 1 else 1 - which
                self.send(self.part(self.order[:2], half=half), 5 + which, self.order[2], s, 4)

        def three_on(self):
            first, d = self.order[:2], self.order[2]
            arrived(self.part(first), (self.key, 5))
            for s in (1, -1):
                self.send(self.part(first, {d: -s}, 0 if s == 1 else 1), 7, d, s, 4)

        def near_done(self):
            arrived(self.part(self.order[:2]), (self.key, 6))
            self.across(1)
            self.across(-1)

        def far_done(self):
            arrived(self.part(self.order[:2]), (self.key, 7))
            self.across(2)

        def across(self, which):
            block = self.part(self.order[:-1], {self.order[-1]: which})
            start(block, block, (self.kind, 5), (self.key, 8), partner)

        def from_partner(self):
            arrived(self.part(self.order, core=1 - c), (self.key, 8))

    def first_ring(m):
        ref = lambda p, core, tail: wx.at[m, p["x"], p["z"], p["y"], core, tail]
        return Ring("a", ("a", m), FIRST_ORDERS[m], ref, (0, 64))

    def output_ring(k, h):
        ref = lambda p, core, tail: wu.at[k, p["x"], p["z"], p["y"], core, tail]
        return Ring("u", ("u", k, h), OUTPUT_ORDERS[h], ref, (16 * h, 16))

    def column_ring(k, m):
        ref = lambda p, core, tail: wf.at[k, m, p["z"], p["y"], core, tail]
        return Ring("f", ("f", k, m), COLUMN_ORDERS[k][m], ref, (0, 64))

    def folded_ring(k, m):
        ref = lambda p, core, tail: wp.at[k, m, p["x"], p["z"], p["y"], core, tail]
        return Ring("p", ("p", k, m), FOLDED_ORDERS[k][m], ref, (0, 32))

    A = [first_ring(m) for m in range(3)]
    U = [[output_ring(k, h) for h in range(2)] for k in range(3)]
    F = [[column_ring(k, m) for m in range(3)] for k in range(2)]
    W = [[folded_ring(k, m) for m in range(3)] for k in range(2)]

    def each(rings, step, *rest):
        for ring in rings:
            getattr(ring, step)(*rest)

    def on_x(rings):
        return [r for r in rings if r.order[-1] == "x"]

    def off_x(rings):
        return [r for r in rings if r.order[-1] != "x"]

    barrier = pltpu.get_barrier_semaphore()
    left_sp, right_sp = lax.rem(sp + 31, 32), lax.rem(sp + 1, 32)
    peers = [device(dx=d) for d in (1, 2, 3)]
    peers += [neighbour(d, s) for d in "yz" for s in (1, -1)]
    peers.append(device(dc=1))
    for d in range(4):
        peers += [(right_sp, lax.rem(x + d, 4)), (left_sp, lax.rem(x + d, 4))]
    for peer in peers:
        pl.semaphore_signal(barrier, inc=1, device_id=peer, device_id_type=MESH)
    g_buf[:, pl.ds(0, 8), :] = jnp.zeros((2, 8, 256), F32)
    own = [pltpu.make_async_copy(args[m].at[0], A[m].part(), local.at[m]) for m in range(3)]
    own += [
        pltpu.make_async_copy(args[m].at[pl.ds(1, 2)], wf.at[:, m, z, y, c], local.at[3 + m]) for m in range(3)
    ]
    own.append(pltpu.make_async_copy(w_u, wu.at[:, x, z, y, c], local.at[8]))
    for copy in own:
        copy.start()
    for copy in own:
        copy.wait()
    pl.semaphore_wait(barrier, len(peers))

    outputs = U[0] + U[1] + U[2]
    each(F[0] + outputs, "one")
    each(F[0], "own_two")
    each(A, "one")
    each(A, "own_two")

    def rows_of(xd):
        return 3 * (xd // 2) + 2 * lax.rem(xd, 2), 3 * (xd // 2) + 1, lax.rem(xd, 2)

    def token_copies():
        found = []
        for d in range(4):
            xd = lax.rem(x + d, 4)
            seq_a, seq_b, odd = rows_of(xd)
            row_b = pl.multiple_of(128 * odd, 128)
            here = (sp, xd)
            there = (right_sp, xd)
            pieces = [
                (None, tokens.at[seq_a], x_buf.at[x, pl.ds(A0, ROWS_A)], "a", here),
                (None, tokens.at[seq_b, pl.ds(row_b, ROWS_B)], x_buf.at[x, pl.ds(B0, ROWS_B)], "b", here),
                (sp < 31, tokens.at[seq_a, pl.ds(240, 16)], x_buf.at[x, pl.ds(0, 16)], "ha", there),
                ((odd == 0) & (sp < 31), tokens.at[seq_b, pl.ds(240, 16)], x_buf.at[x, pl.ds(B0 - 16, 16)], "he", there),
                (odd == 1, tokens.at[seq_b, pl.ds(112, 16)], x_buf.at[x, pl.ds(B0 - 16, 16)], "ho", here),
            ]
            for when, src, dst, name, dev in pieces:
                if d == 0 and name in ("a", "b", "ho"):
                    copy = pltpu.make_async_copy(src, dst, local.at[{"a": 6, "b": 7, "ho": 9}[name]])
                    found.append((when, copy, "local"))
                else:
                    group = (name, d) if name in ("he", "ho") else name
                    found.append((when, remote(src, dst, group, name, dev), name))
        return found

    def guarded(when, action):
        if when is None:
            action()
        else:
            pl.when(when)(action)

    t_buf[x] = taps[...]
    for d in (1, 2, 3):
        start(taps, t_buf.at[x], "taps", "taps", device(dx=d))
    token_list = token_copies()

    def start_tokens():
        for when, copy, _ in token_list:
            guarded(when, copy.start)

    def wait_tokens():
        for when, copy, name in token_list:
            if name == "local":
                guarded(when, copy.wait)
        odd = lax.rem(x, 2)
        three, four = pl.ds(0, 3), pl.ds(0, 4)
        for when, dst, name in (
            (None, x_buf.at[three, pl.ds(A0, ROWS_A)], "a"),
            (None, x_buf.at[three, pl.ds(B0, ROWS_B)], "b"),
            (sp > 0, x_buf.at[four, pl.ds(0, 16)], "ha"),
            ((odd == 0) & (sp > 0), x_buf.at[four, pl.ds(B0 - 16, 16)], "he"),
            (odd == 1, x_buf.at[three, pl.ds(B0 - 16, 16)], "ho"),
        ):
            guarded(when, functools.partial(arrived, dst, name))

        @pl.when(sp == 0)
        def _():
            x_buf[:, pl.ds(0, 16), :] = jnp.zeros((4, 16, 512), BF)

        @pl.when((sp == 0) & (odd == 0))
        def _():
            x_buf[:, pl.ds(B0 - 16, 16), :] = jnp.zeros((4, 16, 512), BF)

        arrived(t_buf.at[pl.ds(0, 3)], "taps")

    def normalize(layer):
        def step(r, _):
            rows = pl.ds(pl.multiple_of(r * 32, 32), 32)
            total = jnp.zeros((32, 1), F32)
            for k in range(4):
                v = x_buf[k, rows, :].astype(F32)
                total += jnp.sum(v * v, axis=-1, keepdims=True)
            scale = lax.rsqrt(total * (1.0 / 2048) + EPS)
            for k in range(4):
                v = x_buf[k, rows, :].astype(F32)
                gain = gains[pl.ds(layer, 1), pl.ds(k * 512, 512)]
                n_buf[rows, pl.ds(k * 512, 512)] = (v * scale * gain).astype(BF)
            return 0

        lax.fori_loop(0, ROWS // 32, step, 0)

    def block(b):
        return pl.ds(pl.multiple_of(b * 256, 256), 256)

    def convolve(layer, b, k, outer, inner, value):
        g_buf[k, pl.ds(8, ROWS), :] = inner * value
        tap = t_buf[b, layer].astype(F32)
        conved = jnp.zeros((ROWS, 256), F32)
        for offset in range(3):
            conved += tap[offset : offset + 1, :] * g_buf[k, pl.ds(6 + offset, ROWS), :]
        m_buf[layer % 2, :, block(b)] = (outer * conved).astype(BF)

    def first(m):
        def step(b, _):
            weight = wx[m, b].reshape(2048, 256)
            p_buf[m, :, block(b)] = jnp.dot(n_buf[...], weight, preferred_element_type=F32).astype(BF)
            return 0

        lax.fori_loop(0, 4, step, 0)

    def gate():
        def step(b, _):
            convolve(0, b, 0, *[p_buf[m, :, block(b)].astype(F32) for m in range(3)])
            return 0

        lax.fori_loop(0, 4, step, 0)

    def mix(layer, begin=0, end=4):
        def step(pair, _):
            for k in range(2):
                b = 2 * pair + k

                def project(m):
                    weight = wp[layer - 1, m, b].reshape(1024, 256)
                    got = jnp.dot(m_buf[(layer - 1) % 2], weight, preferred_element_type=F32) * s_buf[...]
                    return got.astype(BF).astype(F32)

                convolve(layer, b, k, project(0), project(1), project(2))
            return 0

        lax.fori_loop(begin // 2, end // 2, step, 0)

    def project_out(layer, b):
        weight = wu[layer, b].reshape(1024, 512)
        return jnp.dot(m_buf[layer % 2], weight, preferred_element_type=F32)

    def scale(layer):
        def step(pair, total):
            for b in (2 * pair, 2 * pair + 1):
                value = project_out(layer - 1, b)
                total += jnp.sum(value * value, axis=-1, keepdims=True)
            return total

        total = lax.fori_loop(0, 2, step, jnp.zeros((ROWS, 1), F32))
        s_buf[...] = jnp.broadcast_to(lax.rsqrt(total * (1.0 / 2048) + EPS), (ROWS, 256))

    def fold(layer):
        for b in range(4):
            columns = pl.ds(b * 512, 512)
            value = wu[layer - 1, b, z, y, c].astype(F32) * gains[pl.ds(layer, 1), columns]
            high = value.astype(BF)
            h_buf[pl.ds(0, 32), columns] = high
            h_buf[pl.ds(32, 32), columns] = (value - high.astype(F32)).astype(BF)

        def step(m, _):
            got = jnp.dot(h_buf[...], wf[layer - 1, m].reshape(2048, 256), preferred_element_type=F32)
            wp[layer - 1, m, x, z, y, c] = (got[:32] + got[32:]).astype(BF)
            return 0

        lax.fori_loop(0, 3, step, 0)

    each([F[1][0]], "one")
    each([F[1][0]], "own_two")
    each([F[1][1]], "one")
    each([F[1][1]], "own_two")
    each([F[1][2]], "one")
    each([F[1][2]], "own_two")
    each([U[0][0]], "one_on", False)
    each([F[0][0], F[0][1]], "one_on")
    each([U[0][1], U[1][0]], "one_on", False)
    each([F[0][2]], "one_on")
    each([U[1][1], U[2][0], U[2][1]], "one_on", False)
    start_tokens()
    each([A[0], A[1], A[2]], "one_on")
    each([U[0][0], U[0][1], U[1][0]], "one_done", False)
    each([U[1][0]], "two_all")
    each([U[1][1]], "one_done", False)
    each([F[1][0]], "one_on")
    each([U[2][0], U[2][1]], "one_done", False)
    each([F[1][1]], "one_on")
    each([F[0][0]], "one_done")
    each([F[1][2]], "one_on")
    each([F[0][1]], "one_done")
    each([U[1][1]], "two_all")
    each([F[0][2], A[0], A[1]], "one_done")
    each([U[0][1]], "two_all")
    each([U[1][0]], "two_on")
    each([F[1][0]], "one_done")
    each([U[2][1]], "two_all")
    each([F[1][1]], "one_done")
    each([F[0][0]], "two_on")
    each([F[1][2]], "one_done")
    each([U[1][1]], "two_on")
    each([F[0][2]], "two_on")
    each([U[0][0]], "two_all")
    each([F[0][1]], "two_on")
    each([U[0][1]], "two_on")
    each([A[0]], "two_on")
    each([U[1][0]], "two_done")
    each([U[2][1]], "two_on")
    each([U[1][0]], "three", 0)
    each([F[1][0], F[1][1]], "two_on")
    each([F[0][0]], "two_done")
    each([F[1][2]], "two_on")
    each([U[1][1]], "two_done")
    each([U[1][0]], "three", 1)
    each([U[0][0]], "two_on")
    each([F[0][2]], "two_done")
    each([U[0][1]], "two_done")
    each([F[0][1]], "two_done")
    each([U[2][1]], "two_done")
    each([F[0][0]], "from_partner")
    each([A[0]], "two_done")
    each([U[1][1]], "three", 0)
    each([A[0]], "three", 0)
    each([A[0]], "three", 1)
    each([F[0][2]], "from_partner")
    each([F[1][0]], "two_done")
    each([U[1][0]], "three_on")
    each([F[0][1]], "from_partner")
    fold(1)
    each([W[0][0]], "one")
    each([W[0][0]], "own_two")
    each([W[0][1]], "one")
    each([W[0][1]], "own_two")
    each([W[0][2]], "one")
    each([W[0][2]], "own_two")
    each([A[2]], "one_done")
    each([F[1][1]], "two_done")
    each([A[1]], "two_on")
    each([U[0][1]], "three", 0)
    each([F[1][2]], "two_done")
    each([U[1][0]], "near_done")
    each([F[1][0]], "from_partner")
    each([U[0][0]], "two_done")
    each([U[0][0]], "three", 0)
    wait_tokens()
    normalize(0)
    each([F[1][1], F[1][2]], "from_partner")
    fold(2)
    each([W[0][2], W[0][0], W[0][1]], "one_on")
    each([W[1][0]], "one")
    each([W[1][0]], "own_two")
    each([W[1][1]], "one")
    each([W[1][1]], "own_two")
    each([W[1][2]], "one")
    each([W[1][2]], "own_two")
    each([A[2]], "two_on")
    each([U[1][0]], "far_done")
    each([U[1][1]], "three_on")
    each([A[0]], "three_on")
    each([U[0][0]], "three", 1)
    each([U[0][0]], "three_on")
    each([U[1][1]], "three", 1)
    each([W[0][2]], "one_done")
    each([U[0][1]], "three_on")
    each([U[1][0]], "from_partner")
    each([W[0][0]], "one_done")
    each([W[1][1]], "one_on")
    each([W[0][1]], "one_done")
    each([W[1][2], W[1][0]], "one_on")
    each([A[2]], "two_done")
    each([A[0]], "near_done")
    each([U[1][1]], "far_done")
    each([A[1]], "two_done")
    each([A[1]], "three", 0)
    each([U[0][0]], "near_done")
    each([U[0][1]], "three", 1)
    each([U[1][1]], "near_done")
    each([W[0][2]], "two_on")
    each([U[0][0]], "far_done")
    each([W[0][0]], "two_on")
    each([W[1][1], W[1][2]], "one_done")
    each([A[2]], "three", 0)
    each([A[1]], "three", 1)
    each([U[0][1]], "far_done")
    each([W[1][0]], "one_done")
    each([A[0]], "far_done")
    each([W[0][1]], "two_on")
    each([U[1][1], U[0][0]], "from_partner")
    each([U[0][1]], "near_done")
    each([W[1][2]], "two_on")
    each([A[1]], "three_on")
    each([W[1][0]], "two_on")
    each([W[0][2]], "two_done")
    each([W[0][2]], "three", 0)
    each([W[0][2]], "three", 1)
    each([W[1][1]], "two_on")
    each([W[0][0]], "two_done")
    each([W[0][0]], "three", 0)
    each([W[0][1]], "two_done")
    each([A[0]], "from_partner")
    first(0)
    each([W[1][2], W[1][0]], "two_done")
    each([U[0][1]], "from_partner")
    each([U[2][0]], "two_all")
    each([A[2], W[0][0]], "three", 1)
    each([W[0][2], A[2]], "three_on")
    each([A[1]], "near_done")
    each([W[1][1]], "two_done")
    each([W[0][1]], "three", 0)
    each([U[2][0]], "two_on")
    each([W[1][1]], "three", 0)
    each([W[0][2]], "near_done")
    each([W[1][0]], "three", 0)
    each([W[1][1]], "three", 1)
    each([W[0][0]], "three_on")
    each([A[1]], "far_done")
    each([W[0][1]], "three", 1)
    each([A[2], W[0][0]], "near_done")
    each([W[0][1]], "three_on")
    each([W[1][2]], "three", 0)
    each([A[1]], "from_partner")
    first(1)
    each([W[0][2]], "far_done")
    each([W[1][0]], "three_on")
    each([W[1][2]], "three", 1)
    each([A[2]], "far_done")
    each([W[1][1]], "three_on")
    each([W[0][1]], "near_done")
    each([U[2][0]], "two_done")
    each([W[1][0]], "three", 1)
    each([U[2][1]], "three", 0)
    each([W[0][2]], "from_partner")
    each([W[1][1]], "near_done")
    each([W[0][1]], "far_done")
    each([W[1][2]], "three_on")
    each([A[2]], "from_partner")
    first(2)
    each([U[2][0]], "three", 0)
    gate()
    each([W[0][0], W[1][0]], "far_done")
    each([W[1][2]], "near_done")
    each([U[2][1], U[2][0]], "three", 1)
    scale(1)
    each([W[0][1]], "from_partner")
    each([W[1][1]], "far_done")
    each([W[0][0]], "from_partner")
    each([W[1][0]], "near_done")
    each([U[2][1]], "three_on")
    mix(1, 0, 2)
    each([W[1][2]], "far_done")
    each([U[2][0]], "three_on")
    mix(1, 2, 4)
    each([W[1][1], W[1][0]], "from_partner")
    each([U[2][0], U[2][1]], "near_done")
    scale(2)
    each([W[1][2]], "from_partner")
    each([U[2][1], U[2][0]], "far_done")
    mix(2, 0, 2)
    mix(2, 2, 4)
    each([U[2][1], U[2][0]], "from_partner")

    seq_a, seq_b, odd = rows_of(x)
    row_b = pl.multiple_of(128 * odd, 128)
    dst_a = out.at[seq_a]
    dst_b = out.at[seq_b, pl.ds(row_b, ROWS_B)]
    for d in (2, 1, 3, 0):
        xd = lax.rem(x + d, 4)
        x_buf[xd] = project_out(L - 1, xd).astype(BF)
        src_a, src_b = x_buf.at[xd, pl.ds(A0, ROWS_A)], x_buf.at[xd, pl.ds(B0, ROWS_B)]
        if d == 0:
            last = [pltpu.make_async_copy(src_a, dst_a, local.at[6]), pltpu.make_async_copy(src_b, dst_b, local.at[7])]
            for copy in last:
                copy.start()
        else:
            start(src_a, dst_a, "out_a", "out_a", (sp, xd))
            start(src_b, dst_b, "out_b", "out_b", (sp, xd))
    three = pl.ds(0, 3)
    two = pl.ds(0, 2)
    for kind, full, lead in (("a", wx, (ALL,)), ("u", wu, (ALL,)), ("p", wp, (ALL, ALL))):
        all_sent(full.at[(*lead, three, 0, 0, 0)], (kind, 1))
        all_sent(full.at[(*lead, two, ALL, 0, 0)], (kind, 2))
        all_sent(full.at[(*lead, ALL, 0, 0, 0)], (kind, 3))
        all_sent(full.at[(*lead, three, ALL, ALL, 0)], (kind, 4))
        all_sent(full.at[(*lead, ALL, ALL, ALL, 0)], (kind, 5))
    all_sent(wf.at[:, :, three, 0, 0], ("f", 1))
    all_sent(wf.at[:, :, two, :, 0], ("f", 2))
    all_sent(wf.at[:, :, :, 0, 0], ("f", 3))
    all_sent(wf.at[:, :, :, :, 0], ("f", 5))
    all_sent(t_buf.at[three], "taps")
    all_sent(x_buf.at[three, pl.ds(A0, ROWS_A)], "a")
    all_sent(x_buf.at[three, pl.ds(B0, ROWS_B)], "b")
    guarded(sp < 31, lambda: all_sent(x_buf.at[:, pl.ds(0, 16)], "ha"))
    for when, copy, name in token_list:
        if name in ("he", "ho"):
            guarded(when, copy.wait_send)
    for wait in (all_sent, arrived):
        wait(out.at[three], "out_a")
        wait(out.at[three, pl.ds(0, ROWS_B)], "out_b")
    for copy in last:
        copy.wait()
    assert max(len(sems.at) - N_RECV, len(sent.at) - N_SEND) <= 0, (len(sems.at), len(sent.at))


def body(tokens, norm_gains, weight_outer, weight_inner, weight_value, conv_taps, weight_output):
    hbm = pl.BlockSpec(memory_space=pl.ANY)
    vmem = pl.BlockSpec(memory_space=pltpu.VMEM)
    result = pl.pallas_call(
        kernel,
        out_shape=jax.ShapeDtypeStruct((6, 256, 512), BF),
        in_specs=[hbm, vmem, hbm, hbm, hbm, vmem, hbm],
        out_specs=hbm,
        scratch_shapes=[
            pltpu.VMEM((3, 4, 4, 4, 2, 64, 256), BF),
            pltpu.VMEM((L, 4, 4, 4, 2, 32, 512), BF),
            pltpu.VMEM((2, 3, 4, 4, 2, 64, 256), BF),
            pltpu.VMEM((2, 3, 4, 4, 4, 2, 32, 256), BF),
            pltpu.VMEM((4, ROWS, 512), BF),
            pltpu.VMEM((ROWS, 2048), BF),
            pltpu.VMEM((2, ROWS, 1024), BF),
            pltpu.VMEM((2, ROWS + 8, 256), F32),
            pltpu.VMEM((4, 3, 3, 256), BF),
            pltpu.VMEM((64, 2048), BF),
            pltpu.VMEM((3, ROWS, 1024), BF),
            pltpu.VMEM((ROWS, 256), F32),
            pltpu.SemaphoreType.DMA((N_SEND,)),
            pltpu.SemaphoreType.DMA((N_RECV,)),
            pltpu.SemaphoreType.DMA((10,)),
        ],
        compiler_params=pltpu.CompilerParams(
            collective_id=0, has_side_effects=True, vmem_limit_bytes=67_000_000
        ),
        name="mixers",
    )(tokens, norm_gains, weight_outer, weight_inner, weight_value, conv_taps, weight_output)
    return result.astype(F32)


def solution(mesh):
    in_specs = (
        P(None, "sp", "tp"),
        P(),
        P(None, "sp", "tp"),
        P(None, "sp", "tp"),
        P(None, "sp", "tp"),
        P(None, None, "tp"),
        P(None, "sp", "tp"),
    )
    out_specs = P(None, "sp", "tp")
    return jax.shard_map(body, mesh=mesh, in_specs=in_specs, out_specs=out_specs, check_vma=False)
```
